32 devices in a mesh: sp: 8 (over z, y), tp: 4 (over x, core).
Axes of the slice: x: 2, y: 2, z: 4, core: 2. Of those that a mesh axis runs over, the one named last changes fastest.
Arguments:
- resid: bfloat16 [2048, 2048], P(('sp', 'tp')), may hold values from -6 to 6
- mix_in: bfloat16 [2048, 512], P('sp', 'tp'), may hold values from -6 to 6
- decay_rate: float32 [32, 64], P('tp'), may hold values from -0.05 to 0, as said below
- turn_rate: float32 [32, 64], P('tp'), may hold values from -3.140625 to 3.140625
- forget: float32 [2048, 32], P('sp', 'tp'), may hold values from -2 to 0, as said below
- input_real: float32 [32, 64, 16], P('tp'), may hold values from -1 to 1
- input_imag: float32 [32, 64, 16], P('tp'), may hold values from -1 to 1
- output_real: float32 [32, 16, 64], P('tp'), may hold values from -0.75 to 0.75
- output_imag: float32 [32, 16, 64], P('tp'), may hold values from -0.75 to 0.75
- skip_gain: float32 [32, 16], P('tp'), may hold values from -5 to 5
- mix_gain: float32 [512], replicated, may hold values from 0.1 to 1.9
- w_out: bfloat16 [512, 2048], replicated, may hold values from -0.25 to 0.25
- ffn_gain: float32 [2048], replicated, may hold values from 0.1 to 1.9
- gating_matrix: bfloat16 [2048, 5632], P('sp', 'tp'), may hold values from -0.125 to 0.125
- w_up: bfloat16 [2048, 5632], P('sp', 'tp'), may hold values from -0.125 to 0.125
- w_down: bfloat16 [5632, 2048], P('tp', 'sp'), may hold values from -0.078125 to 0.078125
Outputs:
- result: bfloat16 [2048, 2048], P(('sp', 'tp'))
The draws below stay inside these ranges and needn't reach their ends.
Inputs may be any that keep to these rules, and one draw needn't show every extreme that they name: `decay_rate`: every entry is negative. `forget`: every entry is at most zero.
All inputs are finite; a program needn't handle non-finite values.
Results may differ from the reference program's by a relative error of at most 0.012.
Values may be sent and summed in bfloat16 or wider, within the bound.
A program may use at most 128 MiB of HBM per device.

```python
import math
import jax
import jax.numpy as jnp
from jax import lax

D = 2048
FF = 5632
GROUPS = 32
CHAN = 16
STATE = 64
TOKENS_PER_SHARD = 256
WIDTH = 512
TOKENS = 2048
N_TP = 4


def draw_decay_rate(key, part):
    k_chooser, k_slow, k_fast = jax.random.split(jax.random.fold_in(key, 11), 3)
    chooser = jax.random.uniform(k_chooser, (GROUPS, 1), jnp.float32)
    keeps = chooser < 0.5
    slow_rate = -jax.random.uniform(k_slow, (GROUPS, STATE), jnp.float32, 0.2, 0.4) / TOKENS
    fast_rate = -jnp.exp(jax.random.uniform(k_fast, (GROUPS, STATE), jnp.float32, math.log(1.0 / 100.0), math.log(1.0 / 30.0)))
    return jnp.where(keeps, slow_rate, fast_rate)


def draw_forget(key, part):
    k_block, jagged_seed, k_where, stack_level_seed = jax.random.split(jax.random.fold_in(key, 23), 4)
    n_blocks = TOKENS // TOKENS_PER_SHARD
    block_rate = jax.random.uniform(k_block, (n_blocks, 1, GROUPS), jnp.float32, 0.05, 0.5) / TOKENS
    roughness = jax.random.uniform(jagged_seed, (n_blocks, TOKENS_PER_SHARD, GROUPS), jnp.float32, 0.5, 1.5)
    settled_hidden = -(block_rate * roughness).reshape(TOKENS, GROUPS)
    placement_lookup = jax.random.randint(k_where, (2, GROUPS), 0, TOKENS)
    stack_index = jnp.log(jax.random.uniform(stack_level_seed, (2, GROUPS), jnp.float32, 0.55, 0.8))
    symbol_offsets = jnp.arange(TOKENS)[:, None, None]
    symbol_clusters = jnp.sum(jnp.where(symbol_offsets == placement_lookup[None], stack_index[None], 0.0), axis=1)
    return settled_hidden + symbol_clusters


def draw_skip_gain(key, part):
    k_size, k_value = jax.random.split(jax.random.fold_in(key, 37))
    level = 0.5 * jnp.exp(math.log(4.0) * jnp.arange(GROUPS, dtype=jnp.float32) / max(GROUPS - 1, 1))[:, None]
    jitter = jax.random.uniform(k_size, (GROUPS, 1), jnp.float32, 0.8, 1.25)
    values = jnp.clip(jax.random.normal(k_value, (GROUPS, CHAN), jnp.float32), -2.0, 2.0)
    return level * jitter * values


def steps_of(own_key, extent, cuts, smallest, top_value):
    def one(dim, shards_of):
        heights = jax.random.uniform(jax.random.fold_in(jax.random.fold_in(own_key, 6), dim), (shards_of,), jnp.float32, smallest / len(cuts), top_value / len(cuts))
        return jnp.repeat(jnp.exp(heights), extent[dim] // shards_of).reshape((-1,) + (1,) * (len(extent) - dim - 1))

    level = one(*cuts[0])
    for cut in cuts[1:]:
        level = level * one(*cut)
    return level


def noise(key, shape, deviation, reach, pieces=(), kind=jnp.bfloat16):
    loudness = steps_of(key, shape, pieces, -0.22, 0.18) if pieces else 1.0
    array = jax.random.normal(key, shape, jnp.float32) * deviation * loudness
    return jnp.minimum(jnp.maximum(array, -reach), reach).astype(kind)


def setup_inputs(seed: int = 0) -> dict:
    key_of = jax.random.split(jax.random.key(seed), 17)
    return {
        "resid": noise(key_of[0], (TOKENS, D), 1.0, 6.0, ((0, 32),)),
        "mix_in": noise(key_of[1], (TOKENS, WIDTH), 1.0, 6.0, ((0, 8), (1, 4))),
        "decay_rate": draw_decay_rate(jax.random.fold_in(key_of[16], 71), 0),
        "turn_rate": jnp.clip(jax.random.uniform(key_of[3], (GROUPS, STATE), jnp.float32, -3.140625, 3.140625), -3.140625, 3.140625),
        "forget": draw_forget(jax.random.fold_in(key_of[16], 71), 0),
        "input_real": noise(key_of[5], (GROUPS, STATE, CHAN), (2 * CHAN) ** -0.5, 1.0, ((0, 4),), jnp.float32),
        "input_imag": noise(key_of[6], (GROUPS, STATE, CHAN), (2 * CHAN) ** -0.5, 1.0, ((0, 4),), jnp.float32),
        "output_real": noise(key_of[7], (GROUPS, CHAN, STATE), STATE ** -0.5, 0.75, ((0, 4),), jnp.float32),
        "output_imag": noise(key_of[8], (GROUPS, CHAN, STATE), STATE ** -0.5, 0.75, ((0, 4),), jnp.float32),
        "skip_gain": draw_skip_gain(jax.random.fold_in(key_of[16], 71), 0),
        "mix_gain": jnp.clip(1.0 + 0.18 * jax.random.normal(key_of[10], (WIDTH,), jnp.float32), 0.1, 1.9),
        "w_out": noise(key_of[11], (WIDTH, D), WIDTH ** -0.5, 0.25),
        "ffn_gain": jnp.clip(1.0 + 0.18 * jax.random.normal(key_of[12], (D,), jnp.float32), 0.1, 1.9),
        "gating_matrix": noise(key_of[13], (D, FF), D ** -0.5, 0.125, ((0, 8), (1, 4))),
        "w_up": noise(key_of[14], (D, FF), D ** -0.5, 0.125, ((0, 8), (1, 4))),
        "w_down": noise(key_of[15], (FF, D), FF ** -0.5, 0.078125, ((0, 4), (1, 8))),
    }


eps = 1e-06

def reference(resid, mix_in, decay_rate, turn_rate, forget, input_real, input_imag, output_real, output_imag, skip_gain, mix_gain, w_out, ffn_gain, gating_matrix, w_up, w_down):
    high = lax.Precision.HIGHEST
    drive = mix_in.astype(jnp.float32).reshape(TOKENS, GROUPS, CHAN)
    in_factor = jnp.sqrt(-jnp.expm1(2.0 * decay_rate))
    feed_real = input_real * in_factor[:, :, None]
    feed_imag = input_imag * in_factor[:, :, None]
    cosine = jnp.cos(turn_rate)
    sine = jnp.sin(turn_rate)

    def advance(carry, inputs):
        real_part, imag_part = carry
        forget_row, drive_row = inputs
        magnitude = jnp.exp(decay_rate + forget_row[:, None])
        step_real = magnitude * cosine
        step_imaginary = magnitude * sine
        push_real = jnp.einsum('gph,gh->gp', feed_real, drive_row, precision=high)
        push_imag = jnp.einsum('gph,gh->gp', feed_imag, drive_row, precision=high)
        new_real = step_real * real_part - step_imaginary * imag_part + push_real
        new_imag = step_real * imag_part + step_imaginary * real_part + push_imag
        response = jnp.einsum('ghp,gp->gh', output_real, new_real, precision=high) - jnp.einsum('ghp,gp->gh', output_imag, new_imag, precision=high) + skip_gain * drive_row
        return ((new_real, new_imag), response)
    zero_state = jnp.zeros((GROUPS, STATE), jnp.float32)
    _, response = lax.scan(advance, (zero_state, zero_state), (forget, drive))
    mixer_out = jax.nn.gelu(response.reshape(TOKENS, WIDTH)).astype(jnp.bfloat16)
    down_parts = w_down.astype(jnp.float32).reshape(N_TP, FF // N_TP, D)
    n_blocks = TOKENS // TOKENS_PER_SHARD

    def finish(inputs):
        mixer_block, resid_block = inputs
        mixed_f = mixer_block.astype(jnp.float32)
        normed = (mixed_f * lax.rsqrt(lax.optimization_barrier(jnp.mean(mixed_f * mixed_f, axis=1, keepdims=True)) + eps) * mix_gain).astype(jnp.bfloat16)
        resid_mid = resid_block.astype(jnp.float32) + jnp.dot(normed, w_out, preferred_element_type=jnp.float32)
        ffn_in = (resid_mid * lax.rsqrt(lax.optimization_barrier(jnp.mean(resid_mid * resid_mid, axis=1, keepdims=True)) + eps) * ffn_gain).astype(jnp.bfloat16)
        gate_val = jnp.dot(ffn_in, gating_matrix, preferred_element_type=jnp.float32)
        up_val = jnp.dot(ffn_in, w_up, preferred_element_type=jnp.float32)
        hidden = (jax.nn.silu(gate_val) * up_val).astype(jnp.bfloat16)
        hidden_parts = hidden.astype(jnp.float32).reshape(TOKENS_PER_SHARD, N_TP, FF // N_TP)
        partial_value = jnp.einsum('tkf,kfd->ktd', hidden_parts, down_parts)
        rounded = lax.optimization_barrier(partial_value.astype(jnp.bfloat16)).astype(jnp.float32)
        ffn = lax.optimization_barrier(jnp.sum(rounded, axis=0))
        return (resid_mid + 0.5 * ffn).astype(jnp.bfloat16)
    result = lax.map(finish, (mixer_out.reshape(n_blocks, TOKENS_PER_SHARD, WIDTH), resid.reshape(n_blocks, TOKENS_PER_SHARD, D)))
    return result.reshape(TOKENS, D)
```

```python
import functools

import jax
import jax.numpy as jnp
from jax import lax
from jax.experimental import pallas as pl
from jax.experimental.pallas import tpu as pltpu
from jax.sharding import PartitionSpec as P

eps = 1e-06


def carried_in(part, axis, combine, identity):
    place = lax.axis_index(axis)
    gathered = jax.tree.map(lambda a: lax.all_gather(a, axis), part)
    state = jax.tree.map(lambda a, e: jnp.zeros_like(a) + jnp.asarray(e, a.dtype), part, identity)

    def one(turn, state):
        return combine(
            state, jax.tree.map(lambda a: lax.dynamic_index_in_dim(a, turn, 0, False), gathered)
        )

    return lax.fori_loop(0, place, one, state)


def chain(earlier, later):
    first_real, first_imag, push_real, push_imag = earlier
    next_real, next_imag, add_real, add_imag = later
    return (
        next_real * first_real - next_imag * first_imag,
        next_real * first_imag + next_imag * first_real,
        next_real * push_real - next_imag * push_imag + add_real,
        next_real * push_imag + next_imag * push_real + add_imag,
    )


def local_states(log_step, push_real, push_imag, turn):
    high = lax.Precision.HIGHEST
    n_rows, columns = log_step.shape
    span = min(32, n_rows)
    n_spans = n_rows // span
    place = jnp.arange(span, dtype=jnp.float32)
    lower = place[:, None] >= place[None, :]
    lower_cube = lower[:, :, None]
    triangle = lower.astype(jnp.float32)
    lag_angle = (place[:, None] - place[None, :])[:, :, None] * turn[None, None, :]
    lag_cos = jnp.where(lower_cube, jnp.cos(lag_angle), 0.0)
    lag_sin = jnp.where(lower_cube, jnp.sin(lag_angle), 0.0)
    ahead = place + 1.0
    own_cos = jnp.cos(ahead[:, None] * turn[None, :])
    own_sin = jnp.sin(ahead[:, None] * turn[None, :])

    def advance(carry, blocks):
        run_log, state_real, state_imag, offset = carry
        log_block, real_block, imag_block = blocks
        inner = jnp.dot(triangle, log_block, precision=high)
        spread = jnp.where(lower_cube, inner[:, None, :] - inner[None, :, :], 0.0)
        weight = jnp.where(lower_cube, jnp.exp(spread), 0.0)
        weight_real = weight * lag_cos
        weight_imag = weight * lag_sin
        new_real = jnp.sum(weight_real * real_block[None] - weight_imag * imag_block[None], axis=1)
        new_imag = jnp.sum(weight_real * imag_block[None] + weight_imag * real_block[None], axis=1)
        fade = jnp.exp(inner)
        carry_real = fade * own_cos
        carry_imag = fade * own_sin
        new_real = new_real + carry_real * state_real[None] - carry_imag * state_imag[None]
        new_imag = new_imag + carry_real * state_imag[None] + carry_imag * state_real[None]
        whole_fade = jnp.exp(run_log[None] + inner)
        whole_angle = (offset + ahead)[:, None] * turn[None, :]
        prefix_real = whole_fade * jnp.cos(whole_angle)
        prefix_imag = whole_fade * jnp.sin(whole_angle)
        following = (run_log + inner[-1], new_real[-1], new_imag[-1], offset + span)
        return (following, (new_real, new_imag, prefix_real, prefix_imag))

    zero_row = jnp.zeros((columns,), jnp.float32)
    start = (zero_row, zero_row, zero_row, jnp.zeros((), jnp.float32))
    blocks = (
        log_step.reshape(n_spans, span, columns),
        push_real.reshape(n_spans, span, columns),
        push_imag.reshape(n_spans, span, columns),
    )
    final, outputs = lax.scan(advance, start, blocks)
    outputs = tuple((item.reshape(n_rows, columns) for item in outputs))
    total_fade = jnp.exp(final[0])
    totals = (
        total_fade * jnp.cos(n_rows * turn),
        total_fade * jnp.sin(n_rows * turn),
        final[1],
        final[2],
    )
    return (outputs, totals)


def plain_device(
    resid,
    mix_in,
    decay_rate,
    turn_rate,
    forget,
    input_real,
    input_imag,
    output_real,
    output_imag,
    skip_gain,
    mix_gain,
    w_out,
    ffn_gain,
    gating_matrix,
    w_up,
    w_down,
):
    high = lax.Precision.HIGHEST
    n_rows, local_width = mix_in.shape
    n_groups, n_state = decay_rate.shape
    n_chan = input_real.shape[2]
    drive = mix_in.astype(jnp.float32).reshape(n_rows, n_groups, n_chan)
    in_factor = jnp.sqrt(-jnp.expm1(2.0 * decay_rate))
    push_real = jnp.einsum(
        "gph,tgh->tgp", input_real * in_factor[:, :, None], drive, precision=high
    ).reshape(n_rows, n_groups * n_state)
    push_imag = jnp.einsum(
        "gph,tgh->tgp", input_imag * in_factor[:, :, None], drive, precision=high
    ).reshape(n_rows, n_groups * n_state)
    log_step = (decay_rate[None] + forget[:, :, None]).reshape(n_rows, n_groups * n_state)
    turn = turn_rate.reshape(n_groups * n_state)
    outputs, totals = local_states(log_step, push_real, push_imag, turn)
    inner_real, inner_imag, prefix_real, prefix_imag = outputs
    ones_row = jnp.ones((n_groups * n_state,), jnp.float32)
    zeroed_row = jnp.zeros((n_groups * n_state,), jnp.float32)
    carry_in = carried_in(totals, "sp", chain, (ones_row, zeroed_row, zeroed_row, zeroed_row))
    state_real = inner_real + prefix_real * carry_in[2][None] - prefix_imag * carry_in[3][None]
    state_imag = inner_imag + prefix_real * carry_in[3][None] + prefix_imag * carry_in[2][None]
    response = (
        jnp.einsum(
            "ghp,tgp->tgh",
            output_real,
            state_real.reshape(n_rows, n_groups, n_state),
            precision=high,
        )
        - jnp.einsum(
            "ghp,tgp->tgh",
            output_imag,
            state_imag.reshape(n_rows, n_groups, n_state),
            precision=high,
        )
        + skip_gain[None] * drive
    )
    mixer_out = jax.nn.gelu(response.reshape(n_rows, local_width)).astype(jnp.bfloat16)
    swapped = lax.all_to_all(mixer_out, "tp", split_axis=0, concat_axis=1, tiled=True)
    mixed_f = swapped.astype(jnp.float32)
    normed = (
        mixed_f * lax.rsqrt(jnp.mean(mixed_f * mixed_f, axis=1, keepdims=True) + eps) * mix_gain
    ).astype(jnp.bfloat16)
    projected = jnp.dot(normed, w_out, preferred_element_type=jnp.float32)
    resid_mid = resid.astype(jnp.float32) + projected
    ffn_in = (
        resid_mid
        * lax.rsqrt(jnp.mean(resid_mid * resid_mid, axis=1, keepdims=True) + eps)
        * ffn_gain
    ).astype(jnp.bfloat16)
    gathered = lax.all_gather(ffn_in, "tp", axis=0, tiled=True)
    gate_val = jnp.dot(
        gathered,
        lax.all_gather(gating_matrix, "sp", axis=0, tiled=True),
        preferred_element_type=jnp.float32,
    )
    up_val = jnp.dot(
        gathered, lax.all_gather(w_up, "sp", axis=0, tiled=True), preferred_element_type=jnp.float32
    )
    hidden = (jax.nn.silu(gate_val) * up_val).astype(jnp.bfloat16)
    partial_value = jnp.dot(
        hidden, lax.all_gather(w_down, "sp", axis=1, tiled=True), preferred_element_type=jnp.float32
    )
    ffn = lax.psum_scatter(
        partial_value.astype(jnp.bfloat16), "tp", scatter_dimension=0, tiled=True
    ).astype(jnp.float32)
    return (resid_mid + 0.5 * ffn).astype(jnp.bfloat16)


MESH = pl.DeviceIdType.MESH
F32 = jnp.float32
BF16 = jnp.bfloat16
HIGH = lax.Precision.HIGHEST


def dot_t(a, b, precision=None):
    return lax.dot_general(
        a, b, (((1,), (1,)), ((), ())), precision=precision, preferred_element_type=F32
    )


def iota(shape, dim):
    return lax.broadcasted_iota(jnp.int32, shape, dim)


def layer_kernel(
    n_sp, n_tp, inner, levels, n_chan, n_state,
    drive_ref, forget_ref, decay_ref, cos_ref, sin_ref,
    feed_re_ref, feed_im_ref, out_re_ref, out_im_ref, skip_ref,
    mix_gain_ref, w_out_ref, ffn_gain_ref, resid_ref, w_ref,
    result_ref,
    s_re, s_im, mag, p_re, p_im, tot, tots, mixed_out, swapped, mid, tokens, weights,
    part, got1, sum1, got2, sum2, got3,
    own_sem, wz_send, wz_recv, wy_send, wy_recv, tot_send, tot_recv, a2a_send, a2a_recv,
    tz_send, tz_recv, tx_send, tx_recv, tc_send, tc_recv,
    c_send, c_recv, x_send, x_recv, z_send, z_recv,
):
    outer = n_sp // inner
    sp = lax.axis_index("sp")
    tp = lax.axis_index("tp")
    z = sp // inner
    y = sp % inner
    x = tp // 2
    c = tp % 2
    n_x = n_tp // 2
    other_x = [((x + e) % n_x) * 2 + c for e in range(n_x)]
    mate = x * 2 + (1 - c)
    n_rows, width = drive_ref.shape
    columns = decay_ref.shape[1]
    own_rows, depth = resid_ref.shape
    piece = weights.shape[2]
    hid = weights.shape[1] // 3

    def remote(src, dst, send, recv, to_sp, to_tp):
        return pltpu.make_async_remote_copy(
            src_ref=src, dst_ref=dst, send_sem=send, recv_sem=recv,
            device_id=(to_sp, to_tp), device_id_type=MESH,
        )

    barrier = pltpu.get_barrier_semaphore()
    for e in range(1, n_sp):
        pl.semaphore_signal(barrier, inc=1, device_id=((sp + e) % n_sp, tp), device_id_type=MESH)
    for e in range(1, n_tp):
        pl.semaphore_signal(barrier, inc=1, device_id=(sp, (tp + e) % n_tp), device_id_type=MESH)
    pl.semaphore_wait(barrier, n_sp + n_tp - 2)

    started = []

    def go(copy):
        copy.start()
        started.append(copy)
        return copy

    def w_across(d):
        to_z = (z + d) % outer
        return remote(
            w_ref.at[to_z], weights.at[sp], wz_send.at[d], wz_recv.at[d], to_z * inner + y, tp
        )

    def w_inner(d, e):
        slot = ((z + outer - d) % outer) * inner + y
        src = w_ref.at[z] if d == 0 else weights.at[slot]
        return remote(
            src, weights.at[slot], wy_send.at[d, e], wy_recv.at[d, e],
            z * inner + (y + e) % inner, tp,
        )

    near = [1] + ([outer - 1] if outer > 2 else [])
    far = [d for d in range(1, outer) if d not in near]
    for e in range(1, inner):
        go(w_inner(0, e))
    crossing = {d: go(w_across(d)) for d in near}
    own = pltpu.make_async_copy(w_ref.at[z], weights.at[sp], own_sem)
    own.start()

    def spread(a, groups):
        low = a.shape[1]
        pick = (iota((low, low * groups), 1) % low == iota((low, low * groups), 0)).astype(F32)
        return jnp.dot(a, pick, precision=HIGH, preferred_element_type=F32)

    n_groups = width // n_chan
    drive = drive_ref[...].astype(F32)
    to_state = iota((columns, width), 0) // n_state == iota((columns, width), 1) // n_chan
    s_re[...] = dot_t(drive, jnp.where(to_state, spread(feed_re_ref[...], n_groups), 0.0), HIGH)
    s_im[...] = dot_t(drive, jnp.where(to_state, spread(feed_im_ref[...], n_groups), 0.0), HIGH)
    group_of = (iota((n_groups, columns), 1) // n_state == iota((n_groups, columns), 0)).astype(F32)
    mag[...] = jnp.exp(
        decay_ref[...]
        + jnp.dot(forget_ref[...], group_of, precision=HIGH, preferred_element_type=F32)
    )

    def scan_block(i, carry):
        cols = pl.ds(pl.multiple_of(i * 128, 128), 128)
        row = iota((n_rows, 128), 0)
        a, re, im = mag[:, cols], s_re[:, cols], s_im[:, cols]
        for k in range(levels):
            shift = 2**k
            inside = row >= shift
            w = jnp.where(inside, a, 0.0)
            w_re = w * cos_ref[k : k + 1, cols]
            w_im = w * sin_ref[k : k + 1, cols]
            b_re = pltpu.roll(re, shift, 0)
            b_im = pltpu.roll(im, shift, 0)
            re = re + w_re * b_re - w_im * b_im
            im = im + w_re * b_im + w_im * b_re
            a = a * jnp.where(inside, pltpu.roll(a, shift, 0), 1.0)
        mag[:, cols] = a
        s_re[:, cols] = re
        s_im[:, cols] = im
        return carry

    lax.fori_loop(0, columns // 128, scan_block, 0)
    last = n_rows - 1
    tot[0:1, :] = mag[last : last + 1, :]
    tot[1:2, :] = s_re[last : last + 1, :]
    tot[2:3, :] = s_im[last : last + 1, :]
    tot[3:8, :] = jnp.zeros((5, columns), F32)
    tots[sp] = tot[...]
    totals = [
        go(remote(tot, tots.at[sp], tot_send.at[e], tot_recv.at[e], (sp + e) % n_sp, tp))
        for e in range(1, n_sp)
    ]
    for d in far:
        crossing[d] = go(w_across(d))

    def prefix_block(i, carry):
        cols = pl.ds(pl.multiple_of(i * 128, 128), 128)
        row = iota((n_rows, 128), 0)
        r_re = jnp.zeros((n_rows, 128), F32) + cos_ref[0:1, cols]
        r_im = jnp.zeros((n_rows, 128), F32) + sin_ref[0:1, cols]
        for k in range(levels):
            bit = (row // 2**k) % 2 == 1
            m_re = jnp.where(bit, cos_ref[k : k + 1, cols], 1.0)
            m_im = jnp.where(bit, sin_ref[k : k + 1, cols], 0.0)
            r_re, r_im = r_re * m_re - r_im * m_im, r_re * m_im + r_im * m_re
        p_re[:, cols] = mag[:, cols] * r_re
        p_im[:, cols] = mag[:, cols] * r_im
        return carry

    lax.fori_loop(0, columns // 128, prefix_block, 0)
    to_chan_re = jnp.where(
        iota((width, columns), 1) // n_state == iota((width, columns), 0) // n_chan,
        spread(out_re_ref[...], n_groups), 0.0)
    to_chan_im = jnp.where(
        iota((width, columns), 1) // n_state == iota((width, columns), 0) // n_chan,
        spread(out_im_ref[...], n_groups), 0.0)
    for copy in totals:
        copy.wait_recv()
    in_re = jnp.zeros((1, columns), F32)
    in_im = jnp.zeros((1, columns), F32)
    full_cos = cos_ref[levels : levels + 1, :]
    full_sin = sin_ref[levels : levels + 1, :]
    for j in range(n_sp):
        there = tots[j]
        t_re = there[0:1] * full_cos
        t_im = there[0:1] * full_sin
        n_re = t_re * in_re - t_im * in_im + there[1:2]
        n_im = t_re * in_im + t_im * in_re + there[2:3]
        earlier = j < sp
        in_re = jnp.where(earlier, n_re, in_re)
        in_im = jnp.where(earlier, n_im, in_im)
    state_re = s_re[...] + p_re[...] * in_re - p_im[...] * in_im
    state_im = s_im[...] + p_re[...] * in_im + p_im[...] * in_re
    response = (
        dot_t(state_re, to_chan_re, HIGH) - dot_t(state_im, to_chan_im, HIGH)
        + skip_ref[...] * drive
    )
    mixed_out[...] = jax.nn.gelu(response).astype(BF16).reshape(n_tp, own_rows, width)
    swaps = []
    for e in range(1, n_tp):
        to = (tp + e) % n_tp
        swaps.append(
            go(remote(mixed_out.at[to], swapped.at[tp], a2a_send.at[e], a2a_recv.at[e], sp, to))
        )
    swapped[tp] = mixed_out[tp]
    inward = []
    for d in near:
        crossing[d].wait_recv()
        for e in range(1, inner):
            inward.append(go(w_inner(d, e)))
    for copy in swaps:
        copy.wait_recv()
    mixed_f = jnp.concatenate([swapped[j] for j in range(n_tp)], axis=1).astype(F32)
    normed = (
        mixed_f
        * lax.rsqrt(jnp.mean(mixed_f * mixed_f, axis=1, keepdims=True) + eps)
        * mix_gain_ref[...]
    ).astype(BF16)
    resid_mid = resid_ref[...].astype(F32) + jnp.dot(
        normed, w_out_ref[...], preferred_element_type=F32
    )
    mid[...] = resid_mid
    home = z * n_tp + tp
    tokens[home] = (
        resid_mid
        * lax.rsqrt(jnp.mean(resid_mid * resid_mid, axis=1, keepdims=True) + eps)
        * ffn_gain_ref[...]
    ).astype(BF16)

    def slot_of(d, who):
        return ((z + outer - d) % outer) * n_tp + who

    def to_x(d, e):
        s = slot_of(d, tp)
        return remote(
            tokens.at[s], tokens.at[s], tx_send.at[d, e], tx_recv.at[d, e], sp, other_x[e]
        )

    def to_mate(d, e):
        s = slot_of(d, other_x[(n_x - e) % n_x])
        return remote(tokens.at[s], tokens.at[s], tc_send.at[d, e], tc_recv.at[d, e], sp, mate)

    t_across = {}
    order = near + far
    for d in order:
        t_across[d] = go(
            remote(
                tokens.at[home], tokens.at[home], tz_send.at[d], tz_recv.at[d],
                ((z + d) % outer) * inner + y, tp,
            )
        )
    arrive_x, arrive_mate = {}, []
    for d in [0] + order:
        if d:
            t_across[d].wait_recv()
        for e in range(1, n_x):
            arrive_x[d, e] = go(to_x(d, e))
        arrive_mate.append(go(to_mate(d, 0)))
    for d in far:
        crossing[d].wait_recv()
        for e in range(1, inner):
            inward.append(go(w_inner(d, e)))
    for d in [0] + order:
        for e in range(1, n_x):
            arrive_x[d, e].wait_recv()
            arrive_mate.append(go(to_mate(d, e)))
    for copy in arrive_mate:
        copy.wait_recv()
    own.wait()
    for e in range(1, inner):
        w_inner(0, e).wait_recv()
    for copy in inward:
        copy.wait_recv()

    def step1(i, k):
        return remote(
            part.at[i, k * 2 + (1 - c)], got1.at[i, k], c_send.at[i, k], c_recv.at[i, k], sp, mate
        )

    def step2(i, e):
        to = (x + e) % n_x
        return remote(
            sum1.at[i, to], got2.at[i, e], x_send.at[i, e], x_recv.at[i, e], sp, to * 2 + c
        )

    def step3(i):
        to_z = (z + i + 1) % outer
        return remote(
            sum2.at[i], got3.at[i], z_send.at[i], z_recv.at[i], to_z * inner + y, tp
        )

    def flow(i, carry):
        @pl.when(i < outer)
        def _():
            to_z = (z + i + 1) % outer
            block = tokens[pl.ds(to_z * n_tp, n_tp)].reshape(n_tp * own_rows, depth)
            both = jnp.zeros((n_tp * own_rows, 2 * hid), F32)
            for k in range(n_sp):
                both += dot_t(block[:, k * piece : (k + 1) * piece], weights[k, 0 : 2 * hid, :])
            hidden = (jax.nn.silu(both[:, :hid]) * both[:, hid:]).astype(BF16)
            for k in range(n_sp):
                value = jnp.dot(hidden, weights[k, 2 * hid :, :], preferred_element_type=F32)
                part[i, :, :, k * piece : (k + 1) * piece] = value.astype(BF16).reshape(
                    n_tp, own_rows, piece
                )
            for k in range(n_x):
                step1(i, k).start()

        @pl.when((i >= 1) & (i < outer + 1))
        def _():
            for k in range(n_x):
                step1(i - 1, k).wait()
                sum1[i - 1, k] = (
                    part[i - 1, k * 2 + c].astype(F32) + got1[i - 1, k].astype(F32)
                ).astype(BF16)
            for e in range(1, n_x):
                step2(i - 1, e).start()

        @pl.when((i >= 2) & (i < outer + 2))
        def _():
            total = sum1[i - 2, x].astype(F32)
            for e in range(1, n_x):
                step2(i - 2, e).wait()
                total += got2[i - 2, e].astype(F32)
            sum2[i - 2] = total.astype(BF16)

            @pl.when(i - 2 < outer - 1)
            def _():
                step3(i - 2).start()

        return carry

    lax.fori_loop(0, outer + 2, flow, 0)
    ffn = sum2[outer - 1].astype(F32)
    for i in range(outer - 1):
        step3(i).wait()
        ffn += got3[i].astype(F32)
    result_ref[...] = (mid[...] + 0.5 * ffn).astype(BF16)
    for copy in started:
        copy.wait_send()


def fused_device(
    n_sp, n_tp, inner,
    resid, mix_in, decay_rate, turn_rate, forget, input_real, input_imag, output_real,
    output_imag, skip_gain, mix_gain, w_out, ffn_gain, gating_matrix, w_up, w_down,
):
    outer = n_sp // inner
    n_rows, width = mix_in.shape
    n_groups, n_state = decay_rate.shape
    n_chan = input_real.shape[2]
    columns = n_groups * n_state
    levels = n_rows.bit_length() - 1
    own_rows, depth = resid.shape
    piece, n_hid = gating_matrix.shape
    hid = n_hid // outer
    in_factor = jnp.sqrt(-jnp.expm1(2.0 * decay_rate))[:, :, None]
    feed_re = (input_real * in_factor).reshape(columns, n_chan)
    feed_im = (input_imag * in_factor).reshape(columns, n_chan)
    powers = 2.0 ** jnp.arange(levels + 1, dtype=F32)
    angle = powers[:, None] * turn_rate.reshape(1, columns)
    w = jnp.concatenate(
        [
            gating_matrix.T.reshape(outer, hid, piece),
            w_up.T.reshape(outer, hid, piece),
            w_down.reshape(outer, hid, piece),
        ],
        axis=1,
    )
    vmem = pl.BlockSpec(memory_space=pltpu.VMEM)
    n_x = n_tp // 2
    dma = pltpu.SemaphoreType.DMA
    wide = pltpu.VMEM((n_rows, columns), F32)
    block = (own_rows, depth)
    return pl.pallas_call(
        functools.partial(layer_kernel, n_sp, n_tp, inner, levels, n_chan, n_state),
        out_shape=jax.ShapeDtypeStruct(resid.shape, BF16),
        in_specs=[vmem] * 14 + [pl.BlockSpec(memory_space=pl.ANY)],
        out_specs=vmem,
        scratch_shapes=[
            wide, wide, wide, wide, wide,
            pltpu.VMEM((8, columns), F32),
            pltpu.VMEM((n_sp, 8, columns), F32),
            pltpu.VMEM((n_tp, own_rows, width), BF16),
            pltpu.VMEM((n_tp, own_rows, width), BF16),
            pltpu.VMEM(block, F32),
            pltpu.VMEM((outer * n_tp,) + block, BF16),
            pltpu.VMEM((n_sp, 3 * hid, piece), BF16),
            pltpu.VMEM((outer, n_tp) + block, BF16),
            pltpu.VMEM((outer, n_x) + block, BF16),
            pltpu.VMEM((outer, n_x) + block, BF16),
            pltpu.VMEM((outer, n_x) + block, BF16),
            pltpu.VMEM((outer,) + block, BF16),
            pltpu.VMEM((outer,) + block, BF16),
            dma, dma((outer,)), dma((outer,)), dma((outer, inner)), dma((outer, inner)),
            dma((n_sp,)), dma((n_sp,)), dma((n_tp,)), dma((n_tp,)),
            dma((outer,)), dma((outer,)), dma((outer, n_x)), dma((outer, n_x)),
            dma((outer, n_x)), dma((outer, n_x)),
            dma((outer, n_x)), dma((outer, n_x)), dma((outer, n_x)), dma((outer, n_x)),
            dma((outer,)), dma((outer,)),
        ],
        compiler_params=pltpu.CompilerParams(
            collective_id=0, has_side_effects=True, vmem_limit_bytes=60 * 2**20
        ),
        name="layer",
    )(
        mix_in, forget, decay_rate.reshape(1, columns), jnp.cos(angle), jnp.sin(angle),
        feed_re, feed_im,
        output_real.reshape(width, n_state), output_imag.reshape(width, n_state),
        skip_gain.reshape(1, width), mix_gain.reshape(1, -1), w_out, ffn_gain.reshape(1, -1),
        resid, w,
    )


def per_device(n_sp, n_tp, *args):
    mix_in, gating_matrix = args[1], args[13]
    inner = 2
    n_rows, width = mix_in.shape
    columns = args[2].shape[0] * args[2].shape[1]
    piece, n_hid = gating_matrix.shape
    fits = (
        n_sp % inner == 0 and n_sp <= 8 and n_tp % 2 == 0
        and n_hid % (16 * (n_sp // inner)) == 0
        and piece % 128 == 0 and width % 128 == 0 and columns % 128 == 0
        and n_rows & (n_rows - 1) == 0
    )
    if fits:
        return fused_device(n_sp, n_tp, inner, *args)
    return plain_device(*args)


def solution(mesh):
    placed = (
        P(("sp", "tp"), None),
        P("sp", "tp"),
        P("tp", None),
        P("tp", None),
        P("sp", "tp"),
        P("tp", None, None),
        P("tp", None, None),
        P("tp", None, None),
        P("tp", None, None),
        P("tp", None),
        P(),
        P(),
        P(),
        P("sp", "tp"),
        P("sp", "tp"),
        P("tp", "sp"),
    )
    return jax.shard_map(
        functools.partial(per_device, mesh.shape["sp"], mesh.shape["tp"]), mesh=mesh, in_specs=placed, out_specs=P(("sp", "tp"), None), check_vma=False
    )
```

```python
import functools

import jax
import jax.numpy as jnp
from jax import lax
from jax.experimental import pallas as pl
from jax.experimental.pallas import tpu as pltpu
from jax.sharding import PartitionSpec as P

eps = 1e-06


def carried_in(part, axis, combine, identity):
    place = lax.axis_index(axis)
    gathered = jax.tree.map(lambda a: lax.all_gather(a, axis), part)
    state = jax.tree.map(lambda a, e: jnp.zeros_like(a) + jnp.asarray(e, a.dtype), part, identity)

    def one(turn, state):
        return combine(
            state, jax.tree.map(lambda a: lax.dynamic_index_in_dim(a, turn, 0, False), gathered)
        )

    return lax.fori_loop(0, place, one, state)


def chain(earlier, later):
    first_real, first_imag, push_real, push_imag = earlier
    next_real, next_imag, add_real, add_imag = later
    return (
        next_real * first_real - next_imag * first_imag,
        next_real * first_imag + next_imag * first_real,
        next_real * push_real - next_imag * push_imag + add_real,
        next_real * push_imag + next_imag * push_real + add_imag,
    )


def local_states(log_step, push_real, push_imag, turn):
    high = lax.Precision.HIGHEST
    n_rows, columns = log_step.shape
    span = min(32, n_rows)
    n_spans = n_rows // span
    place = jnp.arange(span, dtype=jnp.float32)
    lower = place[:, None] >= place[None, :]
    lower_cube = lower[:, :, None]
    triangle = lower.astype(jnp.float32)
    lag_angle = (place[:, None] - place[None, :])[:, :, None] * turn[None, None, :]
    lag_cos = jnp.where(lower_cube, jnp.cos(lag_angle), 0.0)
    lag_sin = jnp.where(lower_cube, jnp.sin(lag_angle), 0.0)
    ahead = place + 1.0
    own_cos = jnp.cos(ahead[:, None] * turn[None, :])
    own_sin = jnp.sin(ahead[:, None] * turn[None, :])

    def advance(carry, blocks):
        run_log, state_real, state_imag, offset = carry
        log_block, real_block, imag_block = blocks
        inner = jnp.dot(triangle, log_block, precision=high)
        spread = jnp.where(lower_cube, inner[:, None, :] - inner[None, :, :], 0.0)
        weight = jnp.where(lower_cube, jnp.exp(spread), 0.0)
        weight_real = weight * lag_cos
        weight_imag = weight * lag_sin
        new_real = jnp.sum(weight_real * real_block[None] - weight_imag * imag_block[None], axis=1)
        new_imag = jnp.sum(weight_real * imag_block[None] + weight_imag * real_block[None], axis=1)
        fade = jnp.exp(inner)
        carry_real = fade * own_cos
        carry_imag = fade * own_sin
        new_real = new_real + carry_real * state_real[None] - carry_imag * state_imag[None]
        new_imag = new_imag + carry_real * state_imag[None] + carry_imag * state_real[None]
        whole_fade = jnp.exp(run_log[None] + inner)
        whole_angle = (offset + ahead)[:, None] * turn[None, :]
        prefix_real = whole_fade * jnp.cos(whole_angle)
        prefix_imag = whole_fade * jnp.sin(whole_angle)
        following = (run_log + inner[-1], new_real[-1], new_imag[-1], offset + span)
        return (following, (new_real, new_imag, prefix_real, prefix_imag))

    zero_row = jnp.zeros((columns,), jnp.float32)
    start = (zero_row, zero_row, zero_row, jnp.zeros((), jnp.float32))
    blocks = (
        log_step.reshape(n_spans, span, columns),
        push_real.reshape(n_spans, span, columns),
        push_imag.reshape(n_spans, span, columns),
    )
    final, outputs = lax.scan(advance, start, blocks)
    outputs = tuple((item.reshape(n_rows, columns) for item in outputs))
    total_fade = jnp.exp(final[0])
    totals = (
        total_fade * jnp.cos(n_rows * turn),
        total_fade * jnp.sin(n_rows * turn),
        final[1],
        final[2],
    )
    return (outputs, totals)


def plain_device(
    resid,
    mix_in,
    decay_rate,
    turn_rate,
    forget,
    input_real,
    input_imag,
    output_real,
    output_imag,
    skip_gain,
    mix_gain,
    w_out,
    ffn_gain,
    gating_matrix,
    w_up,
    w_down,
):
    high = lax.Precision.HIGHEST
    n_rows, local_width = mix_in.shape
    n_groups, n_state = decay_rate.shape
    n_chan = input_real.shape[2]
    drive = mix_in.astype(jnp.float32).reshape(n_rows, n_groups, n_chan)
    in_factor = jnp.sqrt(-jnp.expm1(2.0 * decay_rate))
    push_real = jnp.einsum(
        "gph,tgh->tgp", input_real * in_factor[:, :, None], drive, precision=high
    ).reshape(n_rows, n_groups * n_state)
    push_imag = jnp.einsum(
        "gph,tgh->tgp", input_imag * in_factor[:, :, None], drive, precision=high
    ).reshape(n_rows, n_groups * n_state)
    log_step = (decay_rate[None] + forget[:, :, None]).reshape(n_rows, n_groups * n_state)
    turn = turn_rate.reshape(n_groups * n_state)
    outputs, totals = local_states(log_step, push_real, push_imag, turn)
    inner_real, inner_imag, prefix_real, prefix_imag = outputs
    ones_row = jnp.ones((n_groups * n_state,), jnp.float32)
    zeroed_row = jnp.zeros((n_groups * n_state,), jnp.float32)
    carry_in = carried_in(totals, "sp", chain, (ones_row, zeroed_row, zeroed_row, zeroed_row))
    state_real = inner_real + prefix_real * carry_in[2][None] - prefix_imag * carry_in[3][None]
    state_imag = inner_imag + prefix_real * carry_in[3][None] + prefix_imag * carry_in[2][None]
    response = (
        jnp.einsum(
            "ghp,tgp->tgh",
            output_real,
            state_real.reshape(n_rows, n_groups, n_state),
            precision=high,
        )
        - jnp.einsum(
            "ghp,tgp->tgh",
            output_imag,
            state_imag.reshape(n_rows, n_groups, n_state),
            precision=high,
        )
        + skip_gain[None] * drive
    )
    mixer_out = jax.nn.gelu(response.reshape(n_rows, local_width)).astype(jnp.bfloat16)
    swapped = lax.all_to_all(mixer_out, "tp", split_axis=0, concat_axis=1, tiled=True)
    mixed_f = swapped.astype(jnp.float32)
    normed = (
        mixed_f * lax.rsqrt(jnp.mean(mixed_f * mixed_f, axis=1, keepdims=True) + eps) * mix_gain
    ).astype(jnp.bfloat16)
    projected = jnp.dot(normed, w_out, preferred_element_type=jnp.float32)
    resid_mid = resid.astype(jnp.float32) + projected
    ffn_in = (
        resid_mid
        * lax.rsqrt(jnp.mean(resid_mid * resid_mid, axis=1, keepdims=True) + eps)
        * ffn_gain
    ).astype(jnp.bfloat16)
    gathered = lax.all_gather(ffn_in, "tp", axis=0, tiled=True)
    gate_val = jnp.dot(
        gathered,
        lax.all_gather(gating_matrix, "sp", axis=0, tiled=True),
        preferred_element_type=jnp.float32,
    )
    up_val = jnp.dot(
        gathered, lax.all_gather(w_up, "sp", axis=0, tiled=True), preferred_element_type=jnp.float32
    )
    hidden = (jax.nn.silu(gate_val) * up_val).astype(jnp.bfloat16)
    partial_value = jnp.dot(
        hidden, lax.all_gather(w_down, "sp", axis=1, tiled=True), preferred_element_type=jnp.float32
    )
    ffn = lax.psum_scatter(
        partial_value.astype(jnp.bfloat16), "tp", scatter_dimension=0, tiled=True
    ).astype(jnp.float32)
    return (resid_mid + 0.5 * ffn).astype(jnp.bfloat16)


MESH = pl.DeviceIdType.MESH
F32 = jnp.float32
BF16 = jnp.bfloat16
HIGH = lax.Precision.HIGHEST


def dot_t(a, b, precision=None):
    return lax.dot_general(
        a, b, (((1,), (1,)), ((), ())), precision=precision, preferred_element_type=F32
    )


def iota(shape, dim):
    return lax.broadcasted_iota(jnp.int32, shape, dim)


def one_minus_exp(a):
    series = jnp.ones_like(a)
    for k in range(10, 1, -1):
        series = 1.0 + series * a * (1.0 / k)
    return jnp.where(a > -0.3, -a * series, 1.0 - jnp.exp(a))


def layer_kernel(
    n_sp, n_tp, inner, levels, n_chan, n_state,
    drive_ref, forget_ref, decay_ref, turn_ref,
    feed_re_ref, feed_im_ref, out_re_ref, out_im_ref, skip_ref,
    mix_gain_ref, w_out_ref, ffn_gain_ref, resid_ref, w_ref,
    result_ref,
    cos_ref, sin_ref, s_re, s_im, mag, p_re, p_im, tot, tots, mixed_out, swapped, mid, tokens, weights,
    part, got1, sum1, got2, sum2, got3,
    own_sem, wz_send, wz_recv, wy_send, wy_recv, tot_send, tot_recv, a2a_send, a2a_recv,
    tz_send, tz_recv, tx_send, tx_recv, tc_send, tc_recv,
    c_send, c_recv, x_send, x_recv, z_send, z_recv,
):
    outer = n_sp // inner
    sp = lax.axis_index("sp")
    tp = lax.axis_index("tp")
    z = sp // inner
    y = sp % inner
    x = tp // 2
    c = tp % 2
    n_x = n_tp // 2
    other_x = [((x + e) % n_x) * 2 + c for e in range(n_x)]
    mate = x * 2 + (1 - c)
    n_rows, width = drive_ref.shape
    columns = decay_ref.shape[0] * n_state
    own_rows, depth = resid_ref.shape
    piece = weights.shape[2]
    hid = weights.shape[1] // 3

    def remote(src, dst, send, recv, to_sp, to_tp):
        return pltpu.make_async_remote_copy(
            src_ref=src, dst_ref=dst, send_sem=send, recv_sem=recv,
            device_id=(to_sp, to_tp), device_id_type=MESH,
        )

    barrier = pltpu.get_barrier_semaphore()
    for e in range(1, n_sp):
        pl.semaphore_signal(barrier, inc=1, device_id=((sp + e) % n_sp, tp), device_id_type=MESH)
    for e in range(1, n_tp):
        pl.semaphore_signal(barrier, inc=1, device_id=(sp, (tp + e) % n_tp), device_id_type=MESH)
    pl.semaphore_wait(barrier, n_sp + n_tp - 2)

    started = []

    def go(copy):
        copy.start()
        started.append(copy)
        return copy

    def across(d):
        there = z
        for k in range(outer.bit_length() - 1):
            there += ((d // 2**k) % 2) * (2**k - 2 ** (k + 1) * ((z // 2**k) % 2))
        return there

    def w_across(d):
        to_z = across(d)
        return remote(
            w_ref.at[to_z], weights.at[sp], wz_send.at[d], wz_recv.at[d], to_z * inner + y, tp
        )

    def w_inner(d, e):
        slot = across(d) * inner + y
        src = w_ref.at[z] if d == 0 else weights.at[slot]
        return remote(
            src, weights.at[slot], wy_send.at[d, e], wy_recv.at[d, e],
            z * inner + (y + e) % inner, tp,
        )

    near = [1] + ([outer - 1] if outer > 2 else [])
    far = [d for d in range(1, outer) if d not in near]
    first, rest = near[:1], near[1:]
    for e in range(1, inner):
        go(w_inner(0, e))
    crossing = {d: go(w_across(d)) for d in near}
    own = pltpu.make_async_copy(w_ref.at[z], weights.at[sp], own_sem)
    own.start()

    def spread(a, groups):
        low = a.shape[1]
        pick = (iota((low, low * groups), 1) % low == iota((low, low * groups), 0)).astype(F32)
        return jnp.dot(a, pick, precision=HIGH, preferred_element_type=F32)

    n_groups = width // n_chan
    drive = drive_ref[...].astype(F32)
    group_of = iota((n_groups, columns), 1) // n_state == iota((n_groups, columns), 0)

    def as_row(a, per):
        groups, wide = a.shape[0], a.shape[0] * per
        mine = iota((groups, wide), 1) // per == iota((groups, wide), 0)
        return jnp.sum(jnp.where(mine, spread(a, groups), 0.0), axis=0, keepdims=True)

    decay = as_row(decay_ref[...], n_state)
    turn = as_row(turn_ref[...], n_state)
    rows = cos_ref.shape[0]
    power = jnp.zeros((rows, columns), F32)
    for k in range(levels + 1):
        power = jnp.where(iota((rows, columns), 0) == k, float(2**k), power)
    cos_ref[...] = jnp.cos(power * turn)
    sin_ref[...] = jnp.sin(power * turn)
    in_factor = jnp.sqrt(one_minus_exp(2.0 * decay))
    matching = iota((width, columns), 1) // n_state == iota((width, columns), 0) // n_chan

    def expanded(ref):
        return jnp.where(matching, spread(ref[...], n_groups), 0.0)

    s_re[...] = in_factor * jnp.dot(
        drive, expanded(feed_re_ref), precision=HIGH, preferred_element_type=F32
    )
    s_im[...] = in_factor * jnp.dot(
        drive, expanded(feed_im_ref), precision=HIGH, preferred_element_type=F32
    )
    mag[...] = jnp.exp(
        decay
        + lax.dot_general(
            forget_ref[...], group_of.astype(F32), (((0,), (0,)), ((), ())),
            precision=HIGH, preferred_element_type=F32,
        )
    )

    def scan_block(i, carry):
        cols = pl.ds(pl.multiple_of(i * 128, 128), 128)
        row = iota((n_rows, 128), 0)
        a, re, im = mag[:, cols], s_re[:, cols], s_im[:, cols]
        for k in range(levels):
            shift = 2**k
            inside = row >= shift
            w = jnp.where(inside, a, 0.0)
            w_re = w * cos_ref[k : k + 1, cols]
            w_im = w * sin_ref[k : k + 1, cols]
            b_re = pltpu.roll(re, shift, 0)
            b_im = pltpu.roll(im, shift, 0)
            re = re + w_re * b_re - w_im * b_im
            im = im + w_re * b_im + w_im * b_re
            a = a * jnp.where(inside, pltpu.roll(a, shift, 0), 1.0)
        mag[:, cols] = a
        s_re[:, cols] = re
        s_im[:, cols] = im
        return carry

    lax.fori_loop(0, columns // 128, scan_block, 0)
    last = n_rows - 1
    tot[0:1, :] = mag[last : last + 1, :]
    tot[1:2, :] = s_re[last : last + 1, :]
    tot[2:3, :] = s_im[last : last + 1, :]
    tot[3:8, :] = jnp.zeros((5, columns), F32)
    tots[sp] = tot[...]
    totals = [
        go(remote(tot, tots.at[sp], tot_send.at[e], tot_recv.at[e], (sp + e) % n_sp, tp))
        for e in range(1, n_sp)
    ]
    for d in far:
        crossing[d] = go(w_across(d))

    inward = []
    for d in first:
        crossing[d].wait_recv()
        for e in range(1, inner):
            inward.append(go(w_inner(d, e)))

    def prefix_block(i, carry):
        cols = pl.ds(pl.multiple_of(i * 128, 128), 128)
        row = iota((n_rows, 128), 0)
        r_re = jnp.zeros((n_rows, 128), F32) + cos_ref[0:1, cols]
        r_im = jnp.zeros((n_rows, 128), F32) + sin_ref[0:1, cols]
        for k in range(levels):
            bit = (row // 2**k) % 2 == 1
            m_re = jnp.where(bit, cos_ref[k : k + 1, cols], 1.0)
            m_im = jnp.where(bit, sin_ref[k : k + 1, cols], 0.0)
            r_re, r_im = r_re * m_re - r_im * m_im, r_re * m_im + r_im * m_re
        p_re[:, cols] = mag[:, cols] * r_re
        p_im[:, cols] = mag[:, cols] * r_im
        return carry

    lax.fori_loop(0, columns // 128, prefix_block, 0)
    to_chan_re = expanded(out_re_ref)
    to_chan_im = expanded(out_im_ref)
    skip_row = as_row(skip_ref[...], n_chan)
    for copy in totals:
        copy.wait_recv()
    in_re = jnp.zeros((1, columns), F32)
    in_im = jnp.zeros((1, columns), F32)
    full_cos = cos_ref[levels : levels + 1, :]
    full_sin = sin_ref[levels : levels + 1, :]
    for j in range(n_sp):
        there = tots[j]
        t_re = there[0:1] * full_cos
        t_im = there[0:1] * full_sin
        n_re = t_re * in_re - t_im * in_im + there[1:2]
        n_im = t_re * in_im + t_im * in_re + there[2:3]
        earlier = j < sp
        in_re = jnp.where(earlier, n_re, in_re)
        in_im = jnp.where(earlier, n_im, in_im)
    state_re = s_re[...] + p_re[...] * in_re - p_im[...] * in_im
    state_im = s_im[...] + p_re[...] * in_im + p_im[...] * in_re
    response = (
        dot_t(state_re, to_chan_re, HIGH) - dot_t(state_im, to_chan_im, HIGH)
        + skip_row * drive
    )
    mixed_out[...] = jax.nn.gelu(response).astype(BF16).reshape(n_tp, own_rows, width)
    swaps = []
    for e in range(1, n_tp):
        to = (tp + e) % n_tp
        swaps.append(
            go(remote(mixed_out.at[to], swapped.at[tp], a2a_send.at[e], a2a_recv.at[e], sp, to))
        )
    swapped[tp] = mixed_out[tp]
    for d in rest:
        crossing[d].wait_recv()
        for e in range(1, inner):
            inward.append(go(w_inner(d, e)))
    for copy in swaps:
        copy.wait_recv()
    mixed_f = jnp.concatenate([swapped[j] for j in range(n_tp)], axis=1).astype(F32)
    normed = (
        mixed_f
        * lax.rsqrt(jnp.mean(mixed_f * mixed_f, axis=1, keepdims=True) + eps)
        * mix_gain_ref[...]
    ).astype(BF16)
    resid_mid = resid_ref[...].astype(F32) + jnp.dot(
        normed, w_out_ref[...], preferred_element_type=F32
    )
    mid[...] = resid_mid
    home = z * n_tp + tp
    tokens[home] = (
        resid_mid
        * lax.rsqrt(jnp.mean(resid_mid * resid_mid, axis=1, keepdims=True) + eps)
        * ffn_gain_ref[...]
    ).astype(BF16)

    def slot_of(d, who):
        return across(d) * n_tp + who

    def to_x(d, e):
        s = slot_of(d, tp)
        return remote(
            tokens.at[s], tokens.at[s], tx_send.at[d, e], tx_recv.at[d, e], sp, other_x[e]
        )

    def to_mate(d, e):
        s = slot_of(d, other_x[(n_x - e) % n_x])
        return remote(tokens.at[s], tokens.at[s], tc_send.at[d, e], tc_recv.at[d, e], sp, mate)

    t_across = {}
    order = near + far
    for d in order:
        t_across[d] = go(
            remote(
                tokens.at[home], tokens.at[home], tz_send.at[d], tz_recv.at[d],
                across(d) * inner + y, tp,
            )
        )
    for d in far:
        crossing[d].wait_recv()
        for e in range(1, inner):
            inward.append(go(w_inner(d, e)))
    arrive_x, arrive_mate = {}, []
    for d in [0] + order:
        if d:
            t_across[d].wait_recv()
        for e in range(1, n_x):
            arrive_x[d, e] = go(to_x(d, e))
        arrive_mate.append(go(to_mate(d, 0)))
    for d in [0] + order:
        for e in range(1, n_x):
            arrive_x[d, e].wait_recv()
            arrive_mate.append(go(to_mate(d, e)))
    for copy in arrive_mate:
        copy.wait_recv()
    own.wait()
    for e in range(1, inner):
        w_inner(0, e).wait_recv()
    for copy in inward:
        copy.wait_recv()

    def step1(i, k):
        return remote(
            part.at[i, k * 2 + (1 - c)], got1.at[i, k], c_send.at[i, k], c_recv.at[i, k], sp, mate
        )

    def step2(i, e):
        to = (x + e) % n_x
        return remote(
            sum1.at[i, to], got2.at[i, e], x_send.at[i, e], x_recv.at[i, e], sp, to * 2 + c
        )

    def step3(i):
        to_z = across(outer - 1 - i)
        return remote(
            sum2.at[i], got3.at[i], z_send.at[i], z_recv.at[i], to_z * inner + y, tp
        )

    def flow(i, carry):
        @pl.when(i < outer)
        def _():
            to_z = across(outer - 1 - i)
            block = tokens[pl.ds(to_z * n_tp, n_tp)].reshape(n_tp * own_rows, depth)
            both = jnp.zeros((n_tp * own_rows, 2 * hid), F32)
            for k in range(n_sp):
                both += dot_t(block[:, k * piece : (k + 1) * piece], weights[k, 0 : 2 * hid, :])
            hidden = (jax.nn.silu(both[:, :hid]) * both[:, hid:]).astype(BF16)
            for k in range(n_sp):
                value = jnp.dot(hidden, weights[k, 2 * hid :, :], preferred_element_type=F32)
                part[i, :, :, k * piece : (k + 1) * piece] = value.astype(BF16).reshape(
                    n_tp, own_rows, piece
                )
            for k in range(n_x):
                step1(i, k).start()

        @pl.when((i >= 1) & (i < outer + 1))
        def _():
            for k in range(n_x):
                step1(i - 1, k).wait()
                sum1[i - 1, k] = (
                    part[i - 1, k * 2 + c].astype(F32) + got1[i - 1, k].astype(F32)
                ).astype(BF16)
            for e in range(1, n_x):
                step2(i - 1, e).start()

        @pl.when((i >= 2) & (i < outer + 2))
        def _():
            total = sum1[i - 2, x].astype(F32)
            for e in range(1, n_x):
                step2(i - 2, e).wait()
                total += got2[i - 2, e].astype(F32)
            sum2[i - 2] = total.astype(BF16)

            @pl.when(i - 2 < outer - 1)
            def _():
                step3(i - 2).start()

        return carry

    lax.fori_loop(0, outer + 2, flow, 0)
    ffn = sum2[outer - 1].astype(F32)
    for i in range(outer - 1):
        step3(i).wait()
        ffn += got3[i].astype(F32)
    result_ref[...] = (mid[...] + 0.5 * ffn).astype(BF16)
    for copy in started:
        copy.wait_send()


def fused_device(
    n_sp, n_tp, inner,
    resid, mix_in, decay_rate, turn_rate, forget, input_real, input_imag, output_real,
    output_imag, skip_gain, mix_gain, w_out, ffn_gain, gating_matrix, w_up, w_down,
):
    outer = n_sp // inner
    n_rows, width = mix_in.shape
    n_groups, n_state = decay_rate.shape
    n_chan = input_real.shape[2]
    columns = n_groups * n_state
    levels = n_rows.bit_length() - 1
    own_rows, depth = resid.shape
    piece, n_hid = gating_matrix.shape
    hid = n_hid // outer
    feed_re = jnp.swapaxes(input_real, 1, 2).reshape(width, n_state)
    feed_im = jnp.swapaxes(input_imag, 1, 2).reshape(width, n_state)
    w = jnp.concatenate(
        [
            gating_matrix.T.reshape(outer, hid, piece),
            w_up.T.reshape(outer, hid, piece),
            w_down.reshape(outer, hid, piece),
        ],
        axis=1,
    )
    vmem = pl.BlockSpec(memory_space=pltpu.VMEM)
    n_x = n_tp // 2
    dma = pltpu.SemaphoreType.DMA
    wide = pltpu.VMEM((n_rows, columns), F32)
    block = (own_rows, depth)
    return pl.pallas_call(
        functools.partial(layer_kernel, n_sp, n_tp, inner, levels, n_chan, n_state),
        out_shape=jax.ShapeDtypeStruct(resid.shape, BF16),
        in_specs=[vmem] * 13 + [pl.BlockSpec(memory_space=pl.ANY)],
        out_specs=vmem,
        scratch_shapes=[
            pltpu.VMEM((16, columns), F32), pltpu.VMEM((16, columns), F32),
            wide, wide, wide, wide, wide,
            pltpu.VMEM((8, columns), F32),
            pltpu.VMEM((n_sp, 8, columns), F32),
            pltpu.VMEM((n_tp, own_rows, width), BF16),
            pltpu.VMEM((n_tp, own_rows, width), BF16),
            pltpu.VMEM(block, F32),
            pltpu.VMEM((outer * n_tp,) + block, BF16),
            pltpu.VMEM((n_sp, 3 * hid, piece), BF16),
            pltpu.VMEM((outer, n_tp) + block, BF16),
            pltpu.VMEM((outer, n_x) + block, BF16),
            pltpu.VMEM((outer, n_x) + block, BF16),
            pltpu.VMEM((outer, n_x) + block, BF16),
            pltpu.VMEM((outer,) + block, BF16),
            pltpu.VMEM((outer,) + block, BF16),
            dma, dma((outer,)), dma((outer,)), dma((outer, inner)), dma((outer, inner)),
            dma((n_sp,)), dma((n_sp,)), dma((n_tp,)), dma((n_tp,)),
            dma((outer,)), dma((outer,)), dma((outer, n_x)), dma((outer, n_x)),
            dma((outer, n_x)), dma((outer, n_x)),
            dma((outer, n_x)), dma((outer, n_x)), dma((outer, n_x)), dma((outer, n_x)),
            dma((outer,)), dma((outer,)),
        ],
        compiler_params=pltpu.CompilerParams(
            collective_id=0, has_side_effects=True, vmem_limit_bytes=60 * 2**20
        ),
        name="layer",
    )(
        mix_in, forget.T, decay_rate, turn_rate,
        feed_re, feed_im,
        output_real.reshape(width, n_state), output_imag.reshape(width, n_state),
        skip_gain, mix_gain.reshape(1, -1), w_out, ffn_gain.reshape(1, -1),
        resid, w,
    )


def per_device(n_sp, n_tp, *args):
    mix_in, gating_matrix = args[1], args[13]
    inner = 2
    n_rows, width = mix_in.shape
    columns = args[2].shape[0] * args[2].shape[1]
    piece, n_hid = gating_matrix.shape
    fits = (
        n_sp in (2 * inner, 4 * inner) and n_tp % 2 == 0
        and n_hid % (16 * (n_sp // inner)) == 0
        and piece % 128 == 0 and width % 128 == 0 and columns % 128 == 0
        and n_rows & (n_rows - 1) == 0 and n_rows < 2**15
    )
    if fits:
        return fused_device(n_sp, n_tp, inner, *args)
    return plain_device(*args)


def solution(mesh):
    placed = (
        P(("sp", "tp"), None),
        P("sp", "tp"),
        P("tp", None),
        P("tp", None),
        P("sp", "tp"),
        P("tp", None, None),
        P("tp", None, None),
        P("tp", None, None),
        P("tp", None, None),
        P("tp", None),
        P(),
        P(),
        P(),
        P("sp", "tp"),
        P("sp", "tp"),
        P("tp", "sp"),
    )
    return jax.shard_map(
        functools.partial(per_device, mesh.shape["sp"], mesh.shape["tp"]), mesh=mesh, in_specs=placed, out_specs=P(("sp", "tp"), None), check_vma=False
    )
```
